32 devices in a mesh: dp: 4 (over y, x), kv: 4 (over z), tp: 2 (over core).
Axes of the slice: x: 2, y: 2, z: 4, core: 2. Of those that a mesh axis runs over, the one named last changes fastest.
Arguments:
- tokens: bfloat16 [128, 2048], P('dp', ('kv', 'tp')), may hold values from -100 to 100
- delta_state: float32 [128, 8, 128, 128], P(('dp', 'kv'), 'tp'), may hold values from -0.6 to 0.6
- gain_in: bfloat16 [2048], P('kv'), may hold values from 0.099609375 to 1.8984375
- w_query: bfloat16 [2048, 1024], P('kv', 'tp'), may hold values from -0.125 to 0.125
- w_key: bfloat16 [2048, 1024], P('kv', 'tp'), may hold values from -0.125 to 0.125
- w_value: bfloat16 [2048, 1024], P('kv', 'tp'), may hold values from -0.125 to 0.125
- w_out_gate: bfloat16 [2048, 1024], P('kv', 'tp'), may hold values from -0.125 to 0.125
- w_beta: bfloat16 [2048, 8], P('kv'), may hold values from -0.125 to 0.125
- w_decay: bfloat16 [2048, 8], P('kv'), may hold values from -0.125 to 0.125
- decay_rate: float32 [8], P('tp'), may hold values from 0.05 to 3
- head_gain: float32 [128], replicated, may hold values from 0.1 to 1.9
- w_mix: bfloat16 [1024, 2048], P('tp', 'kv'), may hold values from -0.1875 to 0.1875
- gain_mid: bfloat16 [2048], P('kv'), may hold values from 0.099609375 to 1.8984375
- w_gate: bfloat16 [2048, 5632], P('tp', 'kv'), may hold values from -0.125 to 0.125
- w_up: bfloat16 [2048, 5632], P('tp', 'kv'), may hold values from -0.125 to 0.125
- w_down: bfloat16 [5632, 2048], P('kv', 'tp'), may hold values from -0.078125 to 0.078125
Outputs:
- layer_out: bfloat16 [128, 2048], P('dp', ('kv', 'tp'))
- next_state: float32 [128, 8, 128, 128], P(('dp', 'kv'), 'tp')
The draws below stay inside these ranges and needn't reach their ends.
All inputs are finite; a program needn't handle non-finite values.
Results may differ from the reference program's by a relative error of at most 0.0095.
Values may be sent and summed in bfloat16 or wider, within the bound.
A program may use at most 64 MiB of HBM per device.

```python
import math
import jax
import jax.numpy as jnp
from jax import lax

D = 2048
HEADS = 8
HEAD_DIM = 128
FF = 5632
WIDTH = 1024
SEQS = 128
FEAT_DEV = 256
N_KV = 4
N_TP = 2


def draw_tokens(key, part):
    keys = jax.random.split(jax.random.fold_in(key, 7), 3)
    column_pos = jnp.arange(D, dtype=jnp.float32) / max(D - 1, 1)
    core_of = (jnp.arange(D) // FEAT_DEV % N_TP).astype(jnp.float32)
    rough = jax.random.uniform(keys[0], (D,), jnp.float32, 0.7, 1.4)
    column_scale = jnp.exp(jnp.log(3.0) * column_pos + jnp.log(3.0) * core_of) * rough
    row_scale = jnp.exp(jax.random.uniform(keys[1], (SEQS, 1), jnp.float32, jnp.log(0.5), jnp.log(2.0)))
    base = jnp.clip(jax.random.normal(keys[2], (SEQS, D), jnp.float32), -4.0, 4.0)
    values = jnp.clip(base * row_scale * column_scale[None, :], -96.0, 96.0)
    return values.astype(jnp.bfloat16)


def block_scale(own_key, extent, pieces, least, high):
    def one(position, blocks):
        heights = jax.random.uniform(jax.random.fold_in(jax.random.fold_in(own_key, 6), position), (blocks,), jnp.float32, least / len(pieces), high / len(pieces))
        return jnp.repeat(jnp.exp(heights), extent[position] // blocks).reshape((-1,) + (1,) * (len(extent) - position - 1))

    level = one(*pieces[0])
    for cut in pieces[1:]:
        level = level * one(*cut)
    return level


def scatter_about(stream_key, shape, spread, most, cuts=(), kind=jnp.bfloat16):
    drawn = jax.random.normal(stream_key, shape, jnp.float32) * spread
    if len(cuts) > 0:
        drawn = block_scale(stream_key, shape, cuts, -0.22, 0.18) * drawn
    return jnp.clip(drawn, min=-most, max=most).astype(kind)


def setup_inputs(seed: int = 0) -> dict:
    arg_keys = jax.random.split(jax.random.key(seed), 17)
    tokens = draw_tokens(jax.random.fold_in(arg_keys[16], 71), 0)
    delta_state = scatter_about(arg_keys[1], (SEQS, HEADS, HEAD_DIM, HEAD_DIM), 0.1, 0.6, ((0, 16), (1, 2)), jnp.float32)
    gain_in = jnp.clip(1.0 + 0.18 * jax.random.normal(arg_keys[2], (D,), jnp.float32), 0.099609375, 1.8984375).astype(jnp.bfloat16)
    w_query = scatter_about(arg_keys[3], (D, WIDTH), D ** -0.5, 0.125, ((0, 4), (1, 2)))
    w_key = scatter_about(arg_keys[4], (D, WIDTH), D ** -0.5, 0.125, ((0, 4), (1, 2)))
    w_value = scatter_about(arg_keys[5], (D, WIDTH), D ** -0.5, 0.125, ((0, 4), (1, 2)))
    w_out_gate = scatter_about(arg_keys[6], (D, WIDTH), D ** -0.5, 0.125, ((0, 4), (1, 2)))
    w_beta = scatter_about(arg_keys[7], (D, HEADS), D ** -0.5, 0.125, ((0, 4),))
    w_decay = scatter_about(arg_keys[8], (D, HEADS), D ** -0.5, 0.125, ((0, 4),))
    decay_rate = jnp.clip(jnp.exp(math.log(3.0) - 4.0943445 * jax.random.uniform(arg_keys[9], (HEADS,), jnp.float32) ** block_scale(arg_keys[9], (HEADS,), ((0, 2),), -0.2, 0.2)), 0.05, 3.0)
    head_gain = jnp.clip(1.0 + 0.18 * jax.random.normal(arg_keys[10], (HEAD_DIM,), jnp.float32), 0.1, 1.9)
    w_mix = scatter_about(arg_keys[11], (WIDTH, D), WIDTH ** -0.5, 0.1875, ((0, 2), (1, 4)))
    gain_mid = jnp.clip(1.0 + 0.18 * jax.random.normal(arg_keys[12], (D,), jnp.float32), 0.099609375, 1.8984375).astype(jnp.bfloat16)
    w_gate = scatter_about(arg_keys[13], (D, FF), D ** -0.5, 0.125, ((0, 2), (1, 4)))
    w_up = scatter_about(arg_keys[14], (D, FF), D ** -0.5, 0.125, ((0, 2), (1, 4)))
    w_down = scatter_about(arg_keys[15], (FF, D), FF ** -0.5, 0.078125, ((0, 4), (1, 2)))
    return dict(tokens=tokens, delta_state=delta_state, gain_in=gain_in, w_query=w_query, w_key=w_key, w_value=w_value, w_out_gate=w_out_gate, w_beta=w_beta, w_decay=w_decay, decay_rate=decay_rate, head_gain=head_gain, w_mix=w_mix, gain_mid=gain_mid, w_gate=w_gate, w_up=w_up, w_down=w_down)


norm_epsilon = 1e-06

def unit_rows(vector):
    return vector * lax.rsqrt(lax.optimization_barrier(jnp.sum(vector * vector, axis=-1, keepdims=True)) + norm_epsilon)

def mixer_core(query_lin, key_lin, value_lin, gate_lin, beta_lin, decay_lin, delta_state, decay_rate, head_gain):
    seq_count = query_lin.shape[0]
    head_count = beta_lin.shape[1]
    shaped = lambda matrix: matrix.reshape(seq_count, head_count, HEAD_DIM)
    query = unit_rows(jax.nn.silu(shaped(query_lin))) * HEAD_DIM ** (-0.5)
    key_vec = unit_rows(jax.nn.silu(shaped(key_lin)))
    value_vec = jax.nn.silu(shaped(value_lin))
    write_rate = jax.nn.sigmoid(beta_lin)
    keep_rate = jnp.exp(-decay_rate[None, :] * jax.nn.softplus(decay_lin))
    recalled = jnp.einsum('bhkv,bhk->bhv', delta_state, key_vec, precision=lax.Precision.HIGHEST)
    correction = write_rate[..., None] * (value_vec - keep_rate[..., None] * recalled)
    next_state = keep_rate[..., None, None] * delta_state + key_vec[..., :, None] * correction[..., None, :]
    readout = jnp.einsum('bhkv,bhk->bhv', next_state, query, precision=lax.Precision.HIGHEST)
    readout = readout * lax.rsqrt(lax.optimization_barrier(jnp.mean(readout * readout, axis=-1, keepdims=True)) + norm_epsilon)
    readout = readout * head_gain * jax.nn.silu(shaped(gate_lin))
    return (readout.reshape(seq_count, head_count * HEAD_DIM).astype(jnp.bfloat16), next_state)

def halves_product(left, right):
    span = left.shape[1] // N_TP
    total = jnp.zeros((left.shape[0], right.shape[1]), jnp.float32)
    for half_index in range(N_TP):
        partial_value = jnp.dot(left[:, half_index * span:(half_index + 1) * span], right[half_index * span:(half_index + 1) * span], preferred_element_type=jnp.float32).astype(jnp.bfloat16)
        partial_value = lax.optimization_barrier(partial_value)
        total = total + partial_value.astype(jnp.float32)
    return total

def stored_order(matrix):
    rows = matrix.shape[0]
    return jnp.transpose(matrix.reshape(rows, N_KV, N_TP, FEAT_DEV), (0, 2, 1, 3)).reshape(rows, D)

def feature_order(matrix):
    rows = matrix.shape[0]
    return jnp.transpose(matrix.reshape(rows, N_TP, N_KV, FEAT_DEV), (0, 2, 1, 3)).reshape(rows, D)

def reference(tokens, delta_state, gain_in, w_query, w_key, w_value, w_out_gate, w_beta, w_decay, decay_rate, head_gain, w_mix, gain_mid, w_gate, w_up, w_down):
    resid = tokens.astype(jnp.float32)
    row_scale = lax.rsqrt(lax.optimization_barrier(jnp.mean(resid * resid, axis=1)) + norm_epsilon)
    normed = (resid * gain_in.astype(jnp.float32)).astype(jnp.bfloat16)

    def project(weight):
        return jnp.dot(normed, weight, preferred_element_type=jnp.float32) * row_scale[:, None]
    mixed, next_state = mixer_core(project(w_query), project(w_key), project(w_value), project(w_out_gate), project(w_beta), project(w_decay), delta_state, decay_rate, head_gain)
    attn = halves_product(mixed, w_mix)
    middle = (resid + attn).astype(jnp.bfloat16)
    mid_float = middle.astype(jnp.float32)
    mid_scale = lax.rsqrt(lax.optimization_barrier(jnp.mean(mid_float * mid_float, axis=1)) + norm_epsilon)
    normed_mid = (mid_float * gain_mid.astype(jnp.float32)).astype(jnp.bfloat16)
    normed_stored = stored_order(normed_mid)
    gate_part = jnp.dot(normed_stored, w_gate, preferred_element_type=jnp.float32) * mid_scale[:, None]
    up_part = jnp.dot(normed_stored, w_up, preferred_element_type=jnp.float32) * mid_scale[:, None]
    activated = (jax.nn.silu(gate_part) * up_part).astype(jnp.bfloat16)
    down_part = feature_order(jnp.dot(activated, w_down, preferred_element_type=jnp.float32))
    layer_out = (mid_float + down_part).astype(jnp.bfloat16)
    return (layer_out, next_state)
```

```python
import functools
import jax
import jax.numpy as jnp
from jax import lax
from jax.experimental import pallas as pl
from jax.experimental.pallas import tpu as pltpu
from jax.sharding import PartitionSpec as P

D = 2048
HEAD_DIM = 128


norm_epsilon = 1e-06


def unit_rows(vector):
    return vector * lax.rsqrt(jnp.sum(vector * vector, axis=-1, keepdims=True) + norm_epsilon)


def mixer_core(
    query_lin, key_lin, value_lin, gate_lin, beta_lin, decay_lin, delta_state, decay_rate, head_gain
):
    seq_count = query_lin.shape[0]
    head_count = beta_lin.shape[1]
    shaped = lambda matrix: matrix.reshape(seq_count, head_count, HEAD_DIM)
    query = unit_rows(jax.nn.silu(shaped(query_lin))) * HEAD_DIM ** (-0.5)
    key_vec = unit_rows(jax.nn.silu(shaped(key_lin)))
    value_vec = jax.nn.silu(shaped(value_lin))
    write_rate = jax.nn.sigmoid(beta_lin)
    keep_rate = jnp.exp(-decay_rate[None, :] * jax.nn.softplus(decay_lin))
    recalled = jnp.einsum("bhkv,bhk->bhv", delta_state, key_vec, precision=lax.Precision.HIGHEST)
    correction = write_rate[..., None] * (value_vec - keep_rate[..., None] * recalled)
    next_state = (
        keep_rate[..., None, None] * delta_state + key_vec[..., :, None] * correction[..., None, :]
    )
    readout = jnp.einsum("bhkv,bhk->bhv", next_state, query, precision=lax.Precision.HIGHEST)
    readout = readout * lax.rsqrt(
        jnp.mean(readout * readout, axis=-1, keepdims=True) + norm_epsilon
    )
    readout = readout * head_gain * jax.nn.silu(shaped(gate_lin))
    return (readout.reshape(seq_count, head_count * HEAD_DIM).astype(jnp.bfloat16), next_state)


def local(
    tokens,
    delta_state,
    gain_in,
    w_query,
    w_key,
    w_value,
    w_out_gate,
    w_beta,
    w_decay,
    decay_rate,
    head_gain,
    w_mix,
    gain_mid,
    w_gate,
    w_up,
    w_down,
):
    group_size = lax.axis_size("kv")
    group_pos = lax.axis_index("kv")
    core_pos = lax.axis_index("tp")
    all_rows = tokens.shape[0]
    own_rows = all_rows // group_size
    own_first = group_pos * own_rows
    feature_count = tokens.shape[1]
    head_count = w_query.shape[1] // HEAD_DIM
    width_dev = w_query.shape[1]
    token_float = tokens.astype(jnp.float32)
    sum_squares = jnp.sum(token_float * token_float, axis=1, keepdims=True)
    whole_rows, square_pair = (
        lax.all_gather(tokens, "tp", axis=1, tiled=True),
        lax.all_gather(sum_squares.astype(jnp.bfloat16), "tp", axis=1, tiled=True).astype(
            sum_squares.dtype
        ),
    )
    square_total = lax.psum(jnp.sum(square_pair, axis=1), "kv")
    row_scale = lax.rsqrt(square_total / D + norm_epsilon)
    normed = (whole_rows.astype(jnp.float32) * gain_in.astype(jnp.float32)).astype(jnp.bfloat16)
    beta_cols = lax.dynamic_slice_in_dim(w_beta, core_pos * head_count, head_count, 1)
    decay_cols = lax.dynamic_slice_in_dim(w_decay, core_pos * head_count, head_count, 1)
    row_block = normed
    results = [
        jnp.dot(row_block, weight, preferred_element_type=jnp.float32)
        for weight in (w_query, w_key, w_value, w_out_gate, beta_cols, decay_cols)
    ]
    summand = jnp.concatenate(results, axis=1)
    projected = lax.psum_scatter(
        summand.astype(jnp.bfloat16), "kv", scatter_dimension=0, tiled=True
    ).astype(jnp.float32)
    projected = projected * lax.dynamic_slice_in_dim(row_scale, own_first, own_rows, 0)[:, None]
    mixed, next_state = mixer_core(
        projected[:, :width_dev],
        projected[:, width_dev : 2 * width_dev],
        projected[:, 2 * width_dev : 3 * width_dev],
        projected[:, 3 * width_dev : 4 * width_dev],
        projected[:, 4 * width_dev : 4 * width_dev + head_count],
        projected[:, 4 * width_dev + head_count :],
        delta_state,
        decay_rate,
        head_gain,
    )
    attn_part = jnp.dot(
        lax.all_gather(mixed, "kv", axis=0, tiled=True), w_mix, preferred_element_type=jnp.float32
    )
    attn = lax.psum_scatter(
        attn_part.astype(jnp.bfloat16), "tp", scatter_dimension=1, tiled=True
    ).astype(jnp.float32)
    middle_own = (token_float + attn).astype(jnp.bfloat16)
    middle_float = middle_own.astype(jnp.float32)
    mid_squares = jnp.sum(middle_float * middle_float, axis=1, keepdims=True)
    gain_own = lax.dynamic_slice_in_dim(gain_mid, core_pos * feature_count, feature_count, 0)
    normed_own = (middle_float * gain_own.astype(jnp.float32)).astype(jnp.bfloat16)
    normed_half, square_parts = (
        lax.all_gather(normed_own, "kv", axis=1, tiled=True),
        lax.all_gather(mid_squares.astype(jnp.bfloat16), "kv", axis=1, tiled=True).astype(
            mid_squares.dtype
        ),
    )
    mid_total = lax.psum(jnp.sum(square_parts, axis=1), "tp")
    mid_scale = lax.rsqrt(mid_total / D + norm_epsilon)
    hidden_dev = w_gate.shape[1]
    row_block = normed_half
    summand = jnp.concatenate(
        [
            jnp.dot(row_block, w_gate, preferred_element_type=jnp.float32),
            jnp.dot(row_block, w_up, preferred_element_type=jnp.float32),
        ],
        axis=1,
    )
    gate_up = lax.psum(summand.astype(jnp.bfloat16), "tp").astype(jnp.float32)
    gate_up = gate_up * mid_scale[:, None]
    activated = (jax.nn.silu(gate_up[:, :hidden_dev]) * gate_up[:, hidden_dev:]).astype(
        jnp.bfloat16
    )
    down_local = jnp.dot(activated, w_down, preferred_element_type=jnp.float32)
    down_part = lax.psum_scatter(
        down_local.astype(jnp.bfloat16), "kv", scatter_dimension=1, tiled=True
    ).astype(jnp.float32)
    layer_out = (middle_float + down_part).astype(jnp.bfloat16)
    return (layer_out, next_state)


F32 = jnp.float32
BF16 = jnp.bfloat16
MESH = pl.DeviceIdType.MESH


def layer_kernel(
    G,
    decay_rate,
    head_gain,
    gain_in,
    gain_mid,
    tokens,
    delta_state,
    w_query,
    w_key,
    w_value,
    w_out_gate,
    w_beta,
    w_decay,
    w_mix,
    w_gate,
    w_up,
    w_down,
    layer_out,
    next_state,
    tok,
    state,
    wq,
    wk,
    wv,
    wg,
    wb,
    wd,
    wm,
    wgate,
    wup,
    wdown,
    part,
    proj_out,
    proj_in,
    extra_out,
    extra_in,
    gain_out,
    gain_all,
    col_k,
    col_q,
    vec,
    mixed_all,
    attn_out,
    attn_in,
    mid_all,
    middle,
    acc,
    gu_out,
    gu_in,
    sq_out,
    sq_in,
    down_out,
    down_in,
    out_buf,
    load_sem,
    tok_sem,
    gain_sem,
    proj_sem,
    extra_sem,
    mixed_sem,
    attn_sem,
    mid_sem,
    gu_sem,
    sq_sem,
    down_sem,
    store_sem,
):
    k = lax.axis_index("kv")
    t = lax.axis_index("tp")
    other = 1 - t
    R, F = tokens.shape
    own = R // G
    C = w_query.shape[1]
    H = C // HEAD_DIM
    HEADS = w_beta.shape[1]
    HID = w_gate.shape[1]
    partner = {"tp": other}
    offsets = sorted(range(1, G), key=lambda d: -min(d, G - d))

    def peer(d):
        return lax.rem(k + d, G)

    def source(d):
        return lax.rem(k + G - d, G)

    loads = []

    def load(src, dst):
        copy = pltpu.make_async_copy(src, dst, load_sem.at[len(loads)])
        copy.start()
        loads.append(copy)
        return copy

    def remote(src, dst, sems, slot_send, slot_recv, device):
        return pltpu.make_async_remote_copy(
            src_ref=src,
            dst_ref=dst,
            send_sem=sems.at[0, slot_send],
            recv_sem=sems.at[1, slot_recv],
            device_id=device,
            device_id_type=MESH,
        )

    load_tok = load(tokens, tok.at[t])
    barrier = pltpu.get_barrier_semaphore()
    pl.semaphore_signal(barrier, inc=1, device_id=partner, device_id_type=MESH)
    for d in offsets:
        pl.semaphore_signal(barrier, inc=1, device_id={"kv": peer(d)}, device_id_type=MESH)
    load_proj = [
        load(a, b)
        for a, b in (
            (w_query, wq),
            (w_key, wk),
            (w_value, wv),
            (w_out_gate, wg),
            (w_beta, wb),
            (w_decay, wd),
        )
    ]
    load_state = load(delta_state, state)
    load_mix = load(w_mix, wm)
    load_gate = load(w_gate, wgate)
    load_up = load(w_up, wup)
    load_down = load(w_down, wdown)

    gain_mid_own = gain_mid[:, pl.ds(pl.multiple_of(t * F, F), F)].astype(F32)
    gain_out[...] = jnp.broadcast_to(gain_mid_own, gain_out.shape)
    gain_all[k] = jnp.broadcast_to(gain_mid_own, gain_out.shape)
    load_tok.wait()
    pl.semaphore_wait(barrier, G)

    send_tok = remote(tok.at[t], tok.at[t], tok_sem, 0, 0, partner)
    send_tok.start()
    gain_copies = []
    for d in offsets:
        copy = remote(gain_out, gain_all.at[k], gain_sem, d - 1, d - 1, {"kv": peer(d)})
        copy.start()
        gain_copies.append((d, copy))

    weights = (wq, wk, wv, wg)

    def rows_of(half):
        return pl.ds(pl.multiple_of(half * F, F), F)

    def scaled(half):
        x = tok[half].astype(F32)
        gain = gain_in[:, rows_of(half)].astype(F32)
        return (x * gain).astype(BF16), jnp.sum(x * x, axis=1, keepdims=True)

    x_own, sq_own = scaled(t)
    for copy, i in zip(load_proj, range(6)):
        copy.wait()
        if i < 4:
            part[:, i * C : (i + 1) * C] = jnp.dot(
                x_own, weights[i][rows_of(t), :], preferred_element_type=F32
            )
    beta_own = jnp.dot(x_own, wb[rows_of(t), :], preferred_element_type=F32)
    decay_own = jnp.dot(x_own, wd[rows_of(t), :], preferred_element_type=F32)

    remote(tok.at[t], tok.at[other], tok_sem, 0, 0, partner).wait_recv()
    x_two, sq_two = scaled(other)
    extra = jnp.zeros((R, 128), F32)
    extra_out[...] = extra.reshape(G, own, 128)
    beta = beta_own + jnp.dot(x_two, wb[rows_of(other), :], preferred_element_type=F32)
    decay = decay_own + jnp.dot(x_two, wd[rows_of(other), :], preferred_element_type=F32)
    extra_out[:, :, 0:HEADS] = beta.reshape(G, own, HEADS)
    extra_out[:, :, HEADS : 2 * HEADS] = decay.reshape(G, own, HEADS)
    extra_out[:, :, 2 * HEADS : 2 * HEADS + 1] = (sq_own + sq_two).reshape(G, own, 1)
    proj_copies = []
    for chunk in range(2):
        for j in range(2):
            i = 2 * chunk + j
            cols = slice(i * C, (i + 1) * C)
            value = part[:, cols] + jnp.dot(
                x_two, weights[i][rows_of(other), :], preferred_element_type=F32
            )
            part[:, cols] = value
            proj_out[chunk, :, :, j * C : (j + 1) * C] = value.astype(BF16).reshape(G, own, C)
        for d in offsets:
            copy = remote(
                proj_out.at[chunk, peer(d)],
                proj_in.at[chunk, d - 1],
                proj_sem,
                chunk * (G - 1) + d - 1,
                chunk * (G - 1) + d - 1,
                {"kv": peer(d)},
            )
            copy.start()
            proj_copies.append(copy)
            if chunk == 0:
                copy = remote(
                    extra_out.at[peer(d)], extra_in.at[d - 1], extra_sem, d - 1, d - 1, {"kv": peer(d)}
                )
                copy.start()
                proj_copies.append(copy)
    own_rows = pl.ds(pl.multiple_of(k * own, own), own)
    sum_extra = extra_out[k]
    for d in range(1, G):
        remote(extra_out.at[0], extra_in.at[d - 1], extra_sem, d - 1, d - 1, partner).wait_recv()
        sum_extra = sum_extra + extra_in[d - 1]
    lane = lax.broadcasted_iota(jnp.int32, (own, 128), 1)

    def lane_of(column):
        return jnp.sum(jnp.where(lane == column, sum_extra, 0.0), axis=1, keepdims=True)

    row_scale = lax.rsqrt(lane_of(2 * HEADS) / D + norm_epsilon)

    def chunk_sum(chunk):
        total = part[own_rows, 2 * chunk * C : 2 * (chunk + 1) * C]
        for d in range(1, G):
            remote(
                proj_out.at[chunk, 0],
                proj_in.at[chunk, d - 1],
                proj_sem,
                chunk * (G - 1) + d - 1,
                chunk * (G - 1) + d - 1,
                partner,
            ).wait_recv()
            total = total + proj_in[chunk, d - 1].astype(F32)
        return total * row_scale

    query_key = chunk_sum(0)
    for h in range(H):
        cols = slice(h * HEAD_DIM, (h + 1) * HEAD_DIM)
        query = unit_rows(jax.nn.silu(query_key[:, cols])) * HEAD_DIM ** (-0.5)
        key_vec = unit_rows(jax.nn.silu(query_key[:, C + h * HEAD_DIM : C + (h + 1) * HEAD_DIM]))
        col_q[h] = query.T
        col_k[h] = key_vec.T
        vec[0, h] = jnp.broadcast_to(
            jnp.sum(query * key_vec, axis=1, keepdims=True), (own, HEAD_DIM)
        )
        vec[1, h] = jnp.broadcast_to(jax.nn.sigmoid(lane_of(t * H + h) * row_scale), (own, HEAD_DIM))
        pre = lane_of(HEADS + t * H + h) * row_scale
        softplus = jnp.maximum(pre, 0.0) + jnp.log1p(jnp.exp(-jnp.abs(pre)))
        vec[2, h] = jnp.broadcast_to(jnp.exp(-decay_rate[h] * softplus), (own, HEAD_DIM))
    load_state.wait()

    def recall(h, carry):
        kc, qc = col_k[h], col_q[h]
        recalled, asked = [], []
        for s in range(own):
            block = state[s, h]
            recalled.append(jnp.sum(block * kc[:, s : s + 1], axis=0, keepdims=True))
            asked.append(jnp.sum(block * qc[:, s : s + 1], axis=0, keepdims=True))
        vec[3, h] = jnp.concatenate(recalled, axis=0)
        vec[4, h] = jnp.concatenate(asked, axis=0)
        return carry

    lax.fori_loop(0, H, recall, 0)
    value_gate = chunk_sum(1)
    gain_row = head_gain[...]
    for h in range(H):
        cols = slice(h * HEAD_DIM, (h + 1) * HEAD_DIM)
        value_vec = jax.nn.silu(value_gate[:, cols])
        gate = jax.nn.silu(value_gate[:, C + h * HEAD_DIM : C + (h + 1) * HEAD_DIM])
        keep = vec[2, h]
        correction = vec[1, h] * (value_vec - keep * vec[3, h])
        readout = keep * vec[4, h] + vec[0, h] * correction
        vec[3, h] = correction
        readout = readout * lax.rsqrt(
            jnp.mean(readout * readout, axis=-1, keepdims=True) + norm_epsilon
        )
        mixed_all[k, :, cols] = (readout * gain_row * gate).astype(BF16)
    mixed_copies = []
    for d in offsets:
        copy = remote(
            mixed_all.at[k], mixed_all.at[k], mixed_sem, d - 1, d - 1, {"kv": peer(d)}
        )
        copy.start()
        mixed_copies.append(copy)

    def update(h, carry):
        kc = col_k[h]
        keep, correction = vec[2, h], vec[3, h]
        for s in range(own):
            state[s, h] = (
                keep[s : s + 1] * state[s, h] + kc[:, s : s + 1] * correction[s : s + 1]
            )
        return carry

    lax.fori_loop(0, H, update, 0)
    load_mix.wait()
    for d in range(1, G):
        remote(
            mixed_all.at[k], mixed_all.at[source(d)], mixed_sem, d - 1, d - 1, partner
        ).wait_recv()
    store_state = pltpu.make_async_copy(state, next_state, store_sem.at[0])
    store_state.start()
    mixed = jnp.concatenate([mixed_all[j].astype(F32) for j in range(G)], axis=0).astype(BF16)
    attn_out[...] = jnp.dot(
        mixed, wm[:, pl.ds(pl.multiple_of(other * F, F), F)], preferred_element_type=F32
    ).astype(BF16)
    send_attn = remote(attn_out, attn_in, attn_sem, 0, 0, partner)
    send_attn.start()
    attn = jnp.dot(
        mixed, wm[:, pl.ds(pl.multiple_of(t * F, F), F)], preferred_element_type=F32
    ).astype(BF16)
    send_attn.wait_recv()
    mid = (tok[t].astype(F32) + (attn.astype(F32) + attn_in[...].astype(F32))).astype(BF16)
    middle[...] = mid
    mid_all[k] = mid
    mid_copies = []
    for d in offsets:
        copy = remote(middle, mid_all.at[k], mid_sem, d - 1, d - 1, {"kv": peer(d)})
        copy.start()
        mid_copies.append(copy)

    cut = (HID // 128 + 1) // 2 * 128
    spans = (slice(0, cut), slice(cut, HID))
    squares = jnp.zeros((R, 1), F32)
    load_gate.wait()
    load_up.wait()
    for d, copy in gain_copies:
        remote(gain_out, gain_all.at[source(d)], gain_sem, d - 1, d - 1, partner).wait_recv()
    order = [0] + sorted(range(1, G), key=lambda d: min(d, G - d))
    gu_copies = []
    for position, d in enumerate(order):
        src = source(d) if d else k
        if d:
            remote(middle, mid_all.at[src], mid_sem, d - 1, d - 1, partner).wait_recv()
        x = mid_all[src].astype(F32)
        squares = squares + jnp.sum(x * x, axis=1, keepdims=True)
        x = (x * gain_all[src][0:1]).astype(BF16)
        rows = pl.ds(pl.multiple_of(src * F, F), F)
        last = position == G - 1
        if last:
            sq_out[...] = jnp.broadcast_to(squares, sq_out.shape)
            send_sq = remote(sq_out, sq_in, sq_sem, 0, 0, partner)
            send_sq.start()
        for c, span in enumerate(spans):
            for j, w in enumerate((wgate, wup)):
                value = jnp.dot(x, w[rows, span], preferred_element_type=F32)
                if position:
                    value = acc[j, :, span] + value
                acc[j, :, span] = value
                if last:
                    gu_out[j, :, span] = value.astype(BF16)
            if last:
                copy = remote(
                    gu_out.at[:, :, span], gu_in.at[:, :, span], gu_sem, c, c, partner
                )
                copy.start()
                gu_copies.append(copy)
    send_sq.wait_recv()
    mid_scale = lax.rsqrt((squares + sq_in[:, 0:1]) / D + norm_epsilon)
    pieces = []
    for c, span in enumerate(spans):
        gu_copies[c].wait_recv()
        gate = (acc[0, :, span] + gu_in[0, :, span].astype(F32)) * mid_scale
        up = (acc[1, :, span] + gu_in[1, :, span].astype(F32)) * mid_scale
        pieces.append((jax.nn.silu(gate) * up).astype(BF16))
    load_down.wait()
    down_copies = []
    for d in offsets + [0]:
        dst = peer(d) if d else k
        cols = pl.ds(pl.multiple_of(dst * F, F), F)
        value = sum(
            jnp.dot(piece, wdown[span, cols], preferred_element_type=F32)
            for piece, span in zip(pieces, spans)
        )
        if d:
            down_out[d - 1] = value.astype(BF16)
            copy = remote(
                down_out.at[d - 1], down_in.at[d - 1], down_sem, d - 1, d - 1, {"kv": dst}
            )
            copy.start()
            down_copies.append(copy)
    total = value
    for d in sorted(range(1, G), key=lambda d: min(d, G - d)):
        remote(down_out.at[d - 1], down_in.at[d - 1], down_sem, d - 1, d - 1, partner).wait_recv()
        total = total + down_in[d - 1].astype(F32)
    out_buf[...] = (middle[...].astype(F32) + total).astype(BF16)
    store_out = pltpu.make_async_copy(out_buf, layer_out, store_sem.at[1])
    store_out.start()
    send_tok.wait_send()
    for d, copy in gain_copies:
        copy.wait_send()
    for copy in proj_copies + mixed_copies + mid_copies + gu_copies + down_copies:
        copy.wait_send()
    send_attn.wait_send()
    send_sq.wait_send()
    store_state.wait()
    store_out.wait()


def one_kernel(
    tokens,
    delta_state,
    gain_in,
    w_query,
    w_key,
    w_value,
    w_out_gate,
    w_beta,
    w_decay,
    decay_rate,
    head_gain,
    w_mix,
    gain_mid,
    w_gate,
    w_up,
    w_down,
):
    G = lax.axis_size("kv")
    R, F = tokens.shape
    own = R // G
    C = w_query.shape[1]
    H = C // HEAD_DIM
    HID = w_gate.shape[1]
    vmem = lambda like: pltpu.VMEM(like.shape, like.dtype)
    dma = pltpu.SemaphoreType.DMA
    anywhere = pl.BlockSpec(memory_space=pl.ANY)
    inside = pl.BlockSpec(memory_space=pltpu.VMEM)
    return pl.pallas_call(
        functools.partial(layer_kernel, G),
        out_shape=(
            jax.ShapeDtypeStruct(tokens.shape, BF16),
            jax.ShapeDtypeStruct(delta_state.shape, F32),
        ),
        in_specs=[pl.BlockSpec(memory_space=pltpu.SMEM)] + [inside] * 3 + [anywhere] * 12,
        out_specs=(anywhere, anywhere),
        scratch_shapes=[
            pltpu.VMEM((2, R, F), BF16),
            vmem(delta_state),
            vmem(w_query),
            vmem(w_key),
            vmem(w_value),
            vmem(w_out_gate),
            vmem(w_beta),
            vmem(w_decay),
            vmem(w_mix),
            vmem(w_gate),
            vmem(w_up),
            vmem(w_down),
            pltpu.VMEM((R, 4 * C), F32),
            pltpu.VMEM((2, G, own, 2 * C), BF16),
            pltpu.VMEM((2, G - 1, own, 2 * C), BF16),
            pltpu.VMEM((G, own, 128), F32),
            pltpu.VMEM((G - 1, own, 128), F32),
            pltpu.VMEM((8, F), F32),
            pltpu.VMEM((G, 8, F), F32),
            pltpu.VMEM((H, HEAD_DIM, own), F32),
            pltpu.VMEM((H, HEAD_DIM, own), F32),
            pltpu.VMEM((5, H, own, HEAD_DIM), F32),
            pltpu.VMEM((G, own, C), BF16),
            pltpu.VMEM((R, F), BF16),
            pltpu.VMEM((R, F), BF16),
            pltpu.VMEM((G, R, F), BF16),
            pltpu.VMEM((R, F), BF16),
            pltpu.VMEM((2, R, HID), F32),
            pltpu.VMEM((2, R, HID), BF16),
            pltpu.VMEM((2, R, HID), BF16),
            pltpu.VMEM((R, 128), F32),
            pltpu.VMEM((R, 128), F32),
            pltpu.VMEM((G - 1, R, F), BF16),
            pltpu.VMEM((G - 1, R, F), BF16),
            pltpu.VMEM((R, F), BF16),
            dma((12,)),
            dma((2, 1)),
            dma((2, G - 1)),
            dma((2, 2 * (G - 1))),
            dma((2, G - 1)),
            dma((2, G - 1)),
            dma((2, 1)),
            dma((2, G - 1)),
            dma((2, 2)),
            dma((2, 1)),
            dma((2, G - 1)),
            dma((2,)),
        ],
        compiler_params=pltpu.CompilerParams(
            collective_id=0, has_side_effects=True, vmem_limit_bytes=60 * 2**20
        ),
    )(
        decay_rate,
        head_gain.reshape(1, -1),
        gain_in.reshape(1, -1),
        gain_mid.reshape(1, -1),
        tokens,
        delta_state,
        w_query,
        w_key,
        w_value,
        w_out_gate,
        w_beta,
        w_decay,
        w_mix,
        w_gate,
        w_up,
        w_down,
    )


def step(*args):
    tokens, w_query, w_gate = args[0], args[3], args[13]
    rows, features = tokens.shape
    aligned = features % 128 == 0 and w_gate.shape[1] % 128 == 0
    aligned = aligned and w_query.shape[1] % HEAD_DIM == 0 and w_query.shape[0] == 2 * features
    aligned = aligned and rows % (8 * lax.axis_size("kv")) == 0 and lax.axis_size("tp") == 2
    return one_kernel(*args) if aligned else local(*args)


def solution(mesh):
    in_specs = (
        P("dp", ("kv", "tp")),
        P(("dp", "kv"), "tp", None, None),
        P("kv"),
        P("kv", "tp"),
        P("kv", "tp"),
        P("kv", "tp"),
        P("kv", "tp"),
        P("kv", None),
        P("kv", None),
        P("tp"),
        P(),
        P("tp", "kv"),
        P("kv"),
        P("tp", "kv"),
        P("tp", "kv"),
        P("kv", "tp"),
    )
    out_specs = (P("dp", ("kv", "tp")), P(("dp", "kv"), "tp", None, None))
    return jax.shard_map(step, mesh=mesh, in_specs=in_specs, out_specs=out_specs, check_vma=False)
```

```python
import functools
import jax
import jax.numpy as jnp
from jax import lax
from jax.experimental import pallas as pl
from jax.experimental.pallas import tpu as pltpu
from jax.sharding import PartitionSpec as P

D = 2048
HEAD_DIM = 128


norm_epsilon = 1e-06


def unit_rows(vector):
    return vector * lax.rsqrt(jnp.sum(vector * vector, axis=-1, keepdims=True) + norm_epsilon)


def mixer_core(
    query_lin, key_lin, value_lin, gate_lin, beta_lin, decay_lin, delta_state, decay_rate, head_gain
):
    seq_count = query_lin.shape[0]
    head_count = beta_lin.shape[1]
    shaped = lambda matrix: matrix.reshape(seq_count, head_count, HEAD_DIM)
    query = unit_rows(jax.nn.silu(shaped(query_lin))) * HEAD_DIM ** (-0.5)
    key_vec = unit_rows(jax.nn.silu(shaped(key_lin)))
    value_vec = jax.nn.silu(shaped(value_lin))
    write_rate = jax.nn.sigmoid(beta_lin)
    keep_rate = jnp.exp(-decay_rate[None, :] * jax.nn.softplus(decay_lin))
    recalled = jnp.einsum("bhkv,bhk->bhv", delta_state, key_vec, precision=lax.Precision.HIGHEST)
    correction = write_rate[..., None] * (value_vec - keep_rate[..., None] * recalled)
    next_state = (
        keep_rate[..., None, None] * delta_state + key_vec[..., :, None] * correction[..., None, :]
    )
    readout = jnp.einsum("bhkv,bhk->bhv", next_state, query, precision=lax.Precision.HIGHEST)
    readout = readout * lax.rsqrt(
        jnp.mean(readout * readout, axis=-1, keepdims=True) + norm_epsilon
    )
    readout = readout * head_gain * jax.nn.silu(shaped(gate_lin))
    return (readout.reshape(seq_count, head_count * HEAD_DIM).astype(jnp.bfloat16), next_state)


def local(
    tokens,
    delta_state,
    gain_in,
    w_query,
    w_key,
    w_value,
    w_out_gate,
    w_beta,
    w_decay,
    decay_rate,
    head_gain,
    w_mix,
    gain_mid,
    w_gate,
    w_up,
    w_down,
):
    group_size = lax.axis_size("kv")
    group_pos = lax.axis_index("kv")
    core_pos = lax.axis_index("tp")
    all_rows = tokens.shape[0]
    own_rows = all_rows // group_size
    own_first = group_pos * own_rows
    feature_count = tokens.shape[1]
    head_count = w_query.shape[1] // HEAD_DIM
    width_dev = w_query.shape[1]
    token_float = tokens.astype(jnp.float32)
    sum_squares = jnp.sum(token_float * token_float, axis=1, keepdims=True)
    whole_rows, square_pair = (
        lax.all_gather(tokens, "tp", axis=1, tiled=True),
        lax.all_gather(sum_squares.astype(jnp.bfloat16), "tp", axis=1, tiled=True).astype(
            sum_squares.dtype
        ),
    )
    square_total = lax.psum(jnp.sum(square_pair, axis=1), "kv")
    row_scale = lax.rsqrt(square_total / D + norm_epsilon)
    normed = (whole_rows.astype(jnp.float32) * gain_in.astype(jnp.float32)).astype(jnp.bfloat16)
    beta_cols = lax.dynamic_slice_in_dim(w_beta, core_pos * head_count, head_count, 1)
    decay_cols = lax.dynamic_slice_in_dim(w_decay, core_pos * head_count, head_count, 1)
    row_block = normed
    results = [
        jnp.dot(row_block, weight, preferred_element_type=jnp.float32)
        for weight in (w_query, w_key, w_value, w_out_gate, beta_cols, decay_cols)
    ]
    summand = jnp.concatenate(results, axis=1)
    projected = lax.psum_scatter(
        summand.astype(jnp.bfloat16), "kv", scatter_dimension=0, tiled=True
    ).astype(jnp.float32)
    projected = projected * lax.dynamic_slice_in_dim(row_scale, own_first, own_rows, 0)[:, None]
    mixed, next_state = mixer_core(
        projected[:, :width_dev],
        projected[:, width_dev : 2 * width_dev],
        projected[:, 2 * width_dev : 3 * width_dev],
        projected[:, 3 * width_dev : 4 * width_dev],
        projected[:, 4 * width_dev : 4 * width_dev + head_count],
        projected[:, 4 * width_dev + head_count :],
        delta_state,
        decay_rate,
        head_gain,
    )
    attn_part = jnp.dot(
        lax.all_gather(mixed, "kv", axis=0, tiled=True), w_mix, preferred_element_type=jnp.float32
    )
    attn = lax.psum_scatter(
        attn_part.astype(jnp.bfloat16), "tp", scatter_dimension=1, tiled=True
    ).astype(jnp.float32)
    middle_own = (token_float + attn).astype(jnp.bfloat16)
    middle_float = middle_own.astype(jnp.float32)
    mid_squares = jnp.sum(middle_float * middle_float, axis=1, keepdims=True)
    gain_own = lax.dynamic_slice_in_dim(gain_mid, core_pos * feature_count, feature_count, 0)
    normed_own = (middle_float * gain_own.astype(jnp.float32)).astype(jnp.bfloat16)
    normed_half, square_parts = (
        lax.all_gather(normed_own, "kv", axis=1, tiled=True),
        lax.all_gather(mid_squares.astype(jnp.bfloat16), "kv", axis=1, tiled=True).astype(
            mid_squares.dtype
        ),
    )
    mid_total = lax.psum(jnp.sum(square_parts, axis=1), "tp")
    mid_scale = lax.rsqrt(mid_total / D + norm_epsilon)
    hidden_dev = w_gate.shape[1]
    row_block = normed_half
    summand = jnp.concatenate(
        [
            jnp.dot(row_block, w_gate, preferred_element_type=jnp.float32),
            jnp.dot(row_block, w_up, preferred_element_type=jnp.float32),
        ],
        axis=1,
    )
    gate_up = lax.psum(summand.astype(jnp.bfloat16), "tp").astype(jnp.float32)
    gate_up = gate_up * mid_scale[:, None]
    activated = (jax.nn.silu(gate_up[:, :hidden_dev]) * gate_up[:, hidden_dev:]).astype(
        jnp.bfloat16
    )
    down_local = jnp.dot(activated, w_down, preferred_element_type=jnp.float32)
    down_part = lax.psum_scatter(
        down_local.astype(jnp.bfloat16), "kv", scatter_dimension=1, tiled=True
    ).astype(jnp.float32)
    layer_out = (middle_float + down_part).astype(jnp.bfloat16)
    return (layer_out, next_state)


F32 = jnp.float32
BF16 = jnp.bfloat16
MESH = pl.DeviceIdType.MESH


def by_column(left, right):
    return lax.dot_general(
        left, right, (((1,), (1,)), ((), ())), preferred_element_type=jnp.float32
    )


def as_row(matrix):
    matrix = matrix.astype(jnp.float32)
    return jnp.concatenate([matrix[i : i + 1] for i in range(matrix.shape[0])], axis=1)


def layer_kernel(
    G,
    decay_rate,
    head_gain,
    gain_in,
    gain_mid,
    tokens,
    delta_state,
    w_query,
    w_key,
    w_value,
    w_out_gate,
    w_beta,
    w_decay,
    w_mix,
    w_gate,
    w_up,
    w_down,
    layer_out,
    next_state,
    tok,
    state,
    wq,
    wk,
    wv,
    wg,
    wb,
    wd,
    wm,
    wgate,
    wup,
    wdown,
    part,
    proj_out,
    proj_in,
    extra_out,
    extra_in,
    gain_out,
    gain_all,
    col_k,
    col_q,
    vec,
    mixed_all,
    attn_out,
    attn_in,
    mid_all,
    middle,
    acc,
    gu_out,
    gu_in,
    sq_out,
    sq_in,
    down_out,
    down_in,
    gain_row_in,
    gain_row_mid,
    load_sem,
    tok_sem,
    gain_sem,
    proj_sem,
    extra_sem,
    mixed_sem,
    attn_sem,
    mid_sem,
    gu_sem,
    sq_sem,
    down_sem,
):
    k = lax.axis_index("kv")
    t = lax.axis_index("tp")
    other = 1 - t
    R, F = tokens.shape
    own = R // G
    C = w_query.shape[1]
    H = C // HEAD_DIM
    HEADS = w_beta.shape[0]
    HID = w_gate.shape[1]
    partner = {"tp": other}
    upper = lax.div(k, G // 2)

    def above(a, b):
        return lax.div(a - b + G - 1, G)

    def far(j):
        down = G - 1 - j
        return (1 - upper) * (down - 1 + above(down, k)) + upper * (j + 1 - above(k, j))

    others = [far(j) for j in range(G - 1)]
    nearest = others[::-1]

    loads = []

    def load(src, dst):
        copy = pltpu.make_async_copy(src, dst, load_sem.at[len(loads)])
        copy.start()
        loads.append(copy)
        return copy

    def remote(src, dst, sems, slot_send, slot_recv, device):
        return pltpu.make_async_remote_copy(
            src_ref=src,
            dst_ref=dst,
            send_sem=sems.at[0, slot_send],
            recv_sem=sems.at[1, slot_recv],
            device_id=device,
            device_id_type=MESH,
        )

    load_tok = load(tokens, tok.at[t])
    barrier = pltpu.get_barrier_semaphore()
    pl.semaphore_signal(barrier, inc=1, device_id=partner, device_id_type=MESH)
    for dst in others:
        pl.semaphore_signal(barrier, inc=1, device_id={"kv": dst}, device_id_type=MESH)
    load_proj = [
        load(a, b)
        for a, b in (
            (w_query, wq),
            (w_key, wk),
            (w_value, wv),
            (w_out_gate, wg),
            (w_beta, wb),
            (w_decay, wd),
        )
    ]

    gain_row_in[...] = as_row(gain_in[...])
    gain_row_mid[...] = as_row(gain_mid[...])
    gain_mid_own = gain_row_mid[:, pl.ds(pl.multiple_of(t * F, F), F)]
    gain_out[...] = jnp.broadcast_to(gain_mid_own, gain_out.shape)
    gain_all[k] = jnp.broadcast_to(gain_mid_own, gain_out.shape)
    load_tok.wait()
    pl.semaphore_wait(barrier, G)

    send_tok = remote(tok.at[t], tok.at[t], tok_sem, 0, 0, partner)
    send_tok.start()
    gain_copies = []
    for j, dst in enumerate(others):
        copy = remote(gain_out, gain_all.at[k], gain_sem, j, k, {"kv": dst})
        copy.start()
        gain_copies.append(copy)

    weights = (wq, wk, wv, wg)

    def rows_of(half):
        return pl.ds(pl.multiple_of(half * F, F), F)

    def scaled(half):
        x = tok[half].astype(F32)
        gain = gain_row_in[:, rows_of(half)]
        return (x * gain).astype(BF16), jnp.sum(x * x, axis=1, keepdims=True)

    x_own, sq_own = scaled(t)
    for copy, i in zip(load_proj, range(6)):
        copy.wait()
        if i < 4:
            part[:, i * C : (i + 1) * C] = jnp.dot(
                x_own, weights[i][rows_of(t), :], preferred_element_type=F32
            )
    load_state = load(delta_state, state)
    load_mix = load(w_mix, wm)
    load_gate = load(w_gate, wgate)
    load_up = load(w_up, wup)
    load_down = load(w_down, wdown)
    beta_own = by_column(x_own, wb[:, rows_of(t)])
    decay_own = by_column(x_own, wd[:, rows_of(t)])

    remote(tok.at[t], tok.at[other], tok_sem, 0, 0, partner).wait_recv()
    x_two, sq_two = scaled(other)
    extra = jnp.zeros((R, 128), F32)
    extra_out[...] = extra.reshape(G, own, 128)
    beta = beta_own + by_column(x_two, wb[:, rows_of(other)])
    decay = decay_own + by_column(x_two, wd[:, rows_of(other)])
    extra_out[:, :, 0:HEADS] = beta.reshape(G, own, HEADS)
    extra_out[:, :, HEADS : 2 * HEADS] = decay.reshape(G, own, HEADS)
    extra_out[:, :, 2 * HEADS : 2 * HEADS + 1] = (sq_own + sq_two).reshape(G, own, 1)
    proj_copies = []
    for chunk in range(2):
        for j in range(2):
            i = 2 * chunk + j
            cols = slice(i * C, (i + 1) * C)
            value = part[:, cols] + jnp.dot(
                x_two, weights[i][rows_of(other), :], preferred_element_type=F32
            )
            part[:, cols] = value
            proj_out[chunk, :, :, j * C : (j + 1) * C] = value.astype(BF16).reshape(G, own, C)
        for j, dst in enumerate(others):
            copy = remote(
                proj_out.at[chunk, dst],
                proj_in.at[chunk, k],
                proj_sem,
                chunk * G + j,
                chunk * G + k,
                {"kv": dst},
            )
            copy.start()
            proj_copies.append(copy)
            if chunk == 0:
                copy = remote(extra_out.at[dst], extra_in.at[k], extra_sem, j, k, {"kv": dst})
                copy.start()
                proj_copies.append(copy)
    own_rows = pl.ds(pl.multiple_of(k * own, own), own)
    sum_extra = extra_out[k]
    for src in nearest:
        remote(extra_out.at[0], extra_in.at[src], extra_sem, 0, src, partner).wait_recv()
        sum_extra = sum_extra + extra_in[src]
    lane = lax.broadcasted_iota(jnp.int32, (own, 128), 1)

    def lane_of(column):
        return jnp.sum(jnp.where(lane == column, sum_extra, 0.0), axis=1, keepdims=True)

    row_scale = lax.rsqrt(lane_of(2 * HEADS) / D + norm_epsilon)

    def chunk_sum(chunk):
        total = part[own_rows, 2 * chunk * C : 2 * (chunk + 1) * C]
        for src in nearest:
            remote(
                proj_out.at[chunk, 0],
                proj_in.at[chunk, src],
                proj_sem,
                chunk * G,
                chunk * G + src,
                partner,
            ).wait_recv()
            total = total + proj_in[chunk, src].astype(F32)
        return total * row_scale

    query_key = chunk_sum(0)
    for h in range(H):
        cols = slice(h * HEAD_DIM, (h + 1) * HEAD_DIM)
        query = unit_rows(jax.nn.silu(query_key[:, cols])) * HEAD_DIM ** (-0.5)
        key_vec = unit_rows(jax.nn.silu(query_key[:, C + h * HEAD_DIM : C + (h + 1) * HEAD_DIM]))
        col_q[h] = query.T
        col_k[h] = key_vec.T
        vec[0, h] = jnp.broadcast_to(
            jnp.sum(query * key_vec, axis=1, keepdims=True), (own, HEAD_DIM)
        )
        vec[1, h] = jnp.broadcast_to(jax.nn.sigmoid(lane_of(t * H + h) * row_scale), (own, HEAD_DIM))
        pre = lane_of(HEADS + t * H + h) * row_scale
        softplus = jnp.maximum(pre, 0.0) + jnp.log1p(jnp.exp(-jnp.abs(pre)))
        vec[2, h] = jnp.broadcast_to(jnp.exp(-decay_rate[h] * softplus), (own, HEAD_DIM))
    load_state.wait()

    def recall(h, carry):
        kc, qc = col_k[h], col_q[h]
        recalled, asked = [], []
        for s in range(own):
            block = state[s, h]
            recalled.append(jnp.sum(block * kc[:, s : s + 1], axis=0, keepdims=True))
            asked.append(jnp.sum(block * qc[:, s : s + 1], axis=0, keepdims=True))
        vec[3, h] = jnp.concatenate(recalled, axis=0)
        vec[4, h] = jnp.concatenate(asked, axis=0)
        return carry

    lax.fori_loop(0, H, recall, 0)
    value_gate = chunk_sum(1)
    gain_row = head_gain[...]
    for h in range(H):
        cols = slice(h * HEAD_DIM, (h + 1) * HEAD_DIM)
        value_vec = jax.nn.silu(value_gate[:, cols])
        gate = jax.nn.silu(value_gate[:, C + h * HEAD_DIM : C + (h + 1) * HEAD_DIM])
        keep = vec[2, h]
        correction = vec[1, h] * (value_vec - keep * vec[3, h])
        readout = keep * vec[4, h] + vec[0, h] * correction
        vec[3, h] = correction
        readout = readout * lax.rsqrt(
            jnp.mean(readout * readout, axis=-1, keepdims=True) + norm_epsilon
        )
        mixed_all[k, :, cols] = (readout * gain_row * gate).astype(BF16)
    mixed_copies = []
    for j, dst in enumerate(others):
        copy = remote(mixed_all.at[k], mixed_all.at[k], mixed_sem, j, k, {"kv": dst})
        copy.start()
        mixed_copies.append(copy)

    def update(h, carry):
        kc = col_k[h]
        keep, correction = vec[2, h], vec[3, h]
        for s in range(own):
            next_state[s, h] = (
                keep[s : s + 1] * state[s, h] + kc[:, s : s + 1] * correction[s : s + 1]
            )
        return carry

    lax.fori_loop(0, H, update, 0)
    load_mix.wait()
    for src in nearest:
        remote(mixed_all.at[k], mixed_all.at[src], mixed_sem, 0, src, partner).wait_recv()
    mixed = jnp.concatenate([mixed_all[j].astype(F32) for j in range(G)], axis=0).astype(BF16)
    attn_out[...] = jnp.dot(
        mixed, wm[:, pl.ds(pl.multiple_of(other * F, F), F)], preferred_element_type=F32
    ).astype(BF16)
    send_attn = remote(attn_out, attn_in, attn_sem, 0, 0, partner)
    send_attn.start()
    attn = jnp.dot(
        mixed, wm[:, pl.ds(pl.multiple_of(t * F, F), F)], preferred_element_type=F32
    ).astype(BF16)
    send_attn.wait_recv()
    mid = (tok[t].astype(F32) + (attn.astype(F32) + attn_in[...].astype(F32))).astype(BF16)
    middle[...] = mid
    mid_all[k] = mid
    mid_copies = []
    for j, dst in enumerate(others):
        copy = remote(middle, mid_all.at[k], mid_sem, j, k, {"kv": dst})
        copy.start()
        mid_copies.append(copy)

    cut = (HID // 128 + 1) // 2 * 128
    spans = (slice(0, cut), slice(cut, HID))
    squares = jnp.zeros((R, 1), F32)
    load_gate.wait()
    load_up.wait()
    for src in nearest:
        remote(gain_out, gain_all.at[src], gain_sem, 0, src, partner).wait_recv()
    gu_copies = []
    for position, src in enumerate([k] + nearest):
        if position:
            remote(middle, mid_all.at[src], mid_sem, 0, src, partner).wait_recv()
        x = mid_all[src].astype(F32)
        squares = squares + jnp.sum(x * x, axis=1, keepdims=True)
        x = (x * gain_all[src][0:1]).astype(BF16)
        rows = pl.ds(pl.multiple_of(src * F, F), F)
        last = position == G - 1
        if last:
            sq_out[...] = jnp.broadcast_to(squares, sq_out.shape)
            send_sq = remote(sq_out, sq_in, sq_sem, 0, 0, partner)
            send_sq.start()
        for c, span in enumerate(spans):
            for j, w in enumerate((wgate, wup)):
                value = jnp.dot(x, w[rows, span], preferred_element_type=F32)
                if position:
                    value = acc[j, :, span] + value
                acc[j, :, span] = value
                if last:
                    gu_out[j, :, span] = value.astype(BF16)
            if last:
                copy = remote(
                    gu_out.at[:, :, span], gu_in.at[:, :, span], gu_sem, c, c, partner
                )
                copy.start()
                gu_copies.append(copy)
    send_sq.wait_recv()
    mid_scale = lax.rsqrt((squares + sq_in[:, 0:1]) / D + norm_epsilon)
    pieces = []
    for c, span in enumerate(spans):
        gu_copies[c].wait_recv()
        gate = (acc[0, :, span] + gu_in[0, :, span].astype(F32)) * mid_scale
        up = (acc[1, :, span] + gu_in[1, :, span].astype(F32)) * mid_scale
        pieces.append((jax.nn.silu(gate) * up).astype(BF16))
    load_down.wait()
    down_copies = []
    for j, dst in enumerate(others + [k]):
        cols = pl.ds(pl.multiple_of(dst * F, F), F)
        value = sum(
            jnp.dot(piece, wdown[span, cols], preferred_element_type=F32)
            for piece, span in zip(pieces, spans)
        )
        if j < G - 1:
            down_out[j] = value.astype(BF16)
            copy = remote(down_out.at[j], down_in.at[k], down_sem, j, k, {"kv": dst})
            copy.start()
            down_copies.append(copy)
    total = value
    for src in nearest:
        remote(down_out.at[0], down_in.at[src], down_sem, 0, src, partner).wait_recv()
        total = total + down_in[src].astype(F32)
    layer_out[...] = (middle[...].astype(F32) + total).astype(BF16)
    send_tok.wait_send()
    for copy in gain_copies + proj_copies + mixed_copies + mid_copies + gu_copies + down_copies:
        copy.wait_send()
    send_attn.wait_send()
    send_sq.wait_send()


def one_kernel(
    tokens,
    delta_state,
    gain_in,
    w_query,
    w_key,
    w_value,
    w_out_gate,
    w_beta,
    w_decay,
    decay_rate,
    head_gain,
    w_mix,
    gain_mid,
    w_gate,
    w_up,
    w_down,
):
    G = lax.axis_size("kv")
    R, F = tokens.shape
    own = R // G
    C = w_query.shape[1]
    H = C // HEAD_DIM
    HID = w_gate.shape[1]
    vmem = lambda like: pltpu.VMEM(like.shape, like.dtype)
    dma = pltpu.SemaphoreType.DMA
    anywhere = pl.BlockSpec(memory_space=pl.ANY)
    inside = pl.BlockSpec(memory_space=pltpu.VMEM)
    return pl.pallas_call(
        functools.partial(layer_kernel, G),
        out_shape=(
            pltpu.VMEM(tokens.shape, BF16),
            pltpu.VMEM(delta_state.shape, F32),
        ),
        in_specs=[pl.BlockSpec(memory_space=pltpu.SMEM)] + [inside] * 3 + [anywhere] * 12,
        out_specs=(inside, inside),
        scratch_shapes=[
            pltpu.VMEM((2, R, F), BF16),
            vmem(delta_state),
            vmem(w_query),
            vmem(w_key),
            vmem(w_value),
            vmem(w_out_gate),
            pltpu.VMEM(w_beta.shape[::-1], BF16),
            pltpu.VMEM(w_decay.shape[::-1], BF16),
            vmem(w_mix),
            vmem(w_gate),
            vmem(w_up),
            vmem(w_down),
            pltpu.VMEM((R, 4 * C), F32),
            pltpu.VMEM((2, G, own, 2 * C), BF16),
            pltpu.VMEM((2, G, own, 2 * C), BF16),
            pltpu.VMEM((G, own, 128), F32),
            pltpu.VMEM((G, own, 128), F32),
            pltpu.VMEM((8, F), F32),
            pltpu.VMEM((G, 8, F), F32),
            pltpu.VMEM((H, HEAD_DIM, own), F32),
            pltpu.VMEM((H, HEAD_DIM, own), F32),
            pltpu.VMEM((5, H, own, HEAD_DIM), F32),
            pltpu.VMEM((G, own, C), BF16),
            pltpu.VMEM((R, F), BF16),
            pltpu.VMEM((R, F), BF16),
            pltpu.VMEM((G, R, F), BF16),
            pltpu.VMEM((R, F), BF16),
            pltpu.VMEM((2, R, HID), F32),
            pltpu.VMEM((2, R, HID), BF16),
            pltpu.VMEM((2, R, HID), BF16),
            pltpu.VMEM((R, 128), F32),
            pltpu.VMEM((R, 128), F32),
            pltpu.VMEM((G - 1, R, F), BF16),
            pltpu.VMEM((G, R, F), BF16),
            pltpu.VMEM((1, 2 * F), F32),
            pltpu.VMEM((1, 2 * F), F32),
            dma((12,)),
            dma((2, 1)),
            dma((2, G)),
            dma((2, 2 * G)),
            dma((2, G)),
            dma((2, G)),
            dma((2, 1)),
            dma((2, G)),
            dma((2, 2)),
            dma((2, 1)),
            dma((2, G)),
        ],
        compiler_params=pltpu.CompilerParams(
            collective_id=0, has_side_effects=True, vmem_limit_bytes=60 * 2**20
        ),
    )(
        decay_rate,
        head_gain.reshape(1, -1),
        gain_in.reshape(-1, 128),
        gain_mid.reshape(-1, 128),
        tokens,
        delta_state,
        w_query,
        w_key,
        w_value,
        w_out_gate,
        w_beta.T,
        w_decay.T,
        w_mix,
        w_gate,
        w_up,
        w_down,
    )


def step(*args):
    tokens, w_query, w_gate = args[0], args[3], args[13]
    rows, features = tokens.shape
    aligned = features % 128 == 0 and w_gate.shape[1] % 128 == 0
    aligned = aligned and w_query.shape[1] % HEAD_DIM == 0 and w_query.shape[0] == 2 * features
    aligned = aligned and rows % (8 * lax.axis_size("kv")) == 0 and lax.axis_size("tp") == 2
    return one_kernel(*args) if aligned else local(*args)


def solution(mesh):
    in_specs = (
        P("dp", ("kv", "tp")),
        P(("dp", "kv"), "tp", None, None),
        P("kv"),
        P("kv", "tp"),
        P("kv", "tp"),
        P("kv", "tp"),
        P("kv", "tp"),
        P("kv", None),
        P("kv", None),
        P("tp"),
        P(),
        P("tp", "kv"),
        P("kv"),
        P("tp", "kv"),
        P("tp", "kv"),
        P("kv", "tp"),
    )
    out_specs = (P("dp", ("kv", "tp")), P(("dp", "kv"), "tp", None, None))
    return jax.shard_map(step, mesh=mesh, in_specs=in_specs, out_specs=out_specs, check_vma=False)
```

```python
import functools
import jax
import jax.numpy as jnp
from jax import lax
from jax.experimental import pallas as pl
from jax.experimental.pallas import tpu as pltpu
from jax.sharding import PartitionSpec as P

D = 2048
HEAD_DIM = 128


norm_epsilon = 1e-06


def unit_rows(vector):
    return vector * lax.rsqrt(jnp.sum(vector * vector, axis=-1, keepdims=True) + norm_epsilon)


def mixer_core(
    query_lin, key_lin, value_lin, gate_lin, beta_lin, decay_lin, delta_state, decay_rate, head_gain
):
    seq_count = query_lin.shape[0]
    head_count = beta_lin.shape[1]
    shaped = lambda matrix: matrix.reshape(seq_count, head_count, HEAD_DIM)
    query = unit_rows(jax.nn.silu(shaped(query_lin))) * HEAD_DIM ** (-0.5)
    key_vec = unit_rows(jax.nn.silu(shaped(key_lin)))
    value_vec = jax.nn.silu(shaped(value_lin))
    write_rate = jax.nn.sigmoid(beta_lin)
    keep_rate = jnp.exp(-decay_rate[None, :] * jax.nn.softplus(decay_lin))
    recalled = jnp.einsum("bhkv,bhk->bhv", delta_state, key_vec, precision=lax.Precision.HIGHEST)
    correction = write_rate[..., None] * (value_vec - keep_rate[..., None] * recalled)
    next_state = (
        keep_rate[..., None, None] * delta_state + key_vec[..., :, None] * correction[..., None, :]
    )
    readout = jnp.einsum("bhkv,bhk->bhv", next_state, query, precision=lax.Precision.HIGHEST)
    readout = readout * lax.rsqrt(
        jnp.mean(readout * readout, axis=-1, keepdims=True) + norm_epsilon
    )
    readout = readout * head_gain * jax.nn.silu(shaped(gate_lin))
    return (readout.reshape(seq_count, head_count * HEAD_DIM).astype(jnp.bfloat16), next_state)


def local(
    tokens,
    delta_state,
    gain_in,
    w_query,
    w_key,
    w_value,
    w_out_gate,
    w_beta,
    w_decay,
    decay_rate,
    head_gain,
    w_mix,
    gain_mid,
    w_gate,
    w_up,
    w_down,
):
    group_size = lax.axis_size("kv")
    group_pos = lax.axis_index("kv")
    core_pos = lax.axis_index("tp")
    all_rows = tokens.shape[0]
    own_rows = all_rows // group_size
    own_first = group_pos * own_rows
    feature_count = tokens.shape[1]
    head_count = w_query.shape[1] // HEAD_DIM
    width_dev = w_query.shape[1]
    token_float = tokens.astype(jnp.float32)
    sum_squares = jnp.sum(token_float * token_float, axis=1, keepdims=True)
    whole_rows, square_pair = (
        lax.all_gather(tokens, "tp", axis=1, tiled=True),
        lax.all_gather(sum_squares.astype(jnp.bfloat16), "tp", axis=1, tiled=True).astype(
            sum_squares.dtype
        ),
    )
    square_total = lax.psum(jnp.sum(square_pair, axis=1), "kv")
    row_scale = lax.rsqrt(square_total / D + norm_epsilon)
    normed = (whole_rows.astype(jnp.float32) * gain_in.astype(jnp.float32)).astype(jnp.bfloat16)
    beta_cols = lax.dynamic_slice_in_dim(w_beta, core_pos * head_count, head_count, 1)
    decay_cols = lax.dynamic_slice_in_dim(w_decay, core_pos * head_count, head_count, 1)
    row_block = normed
    results = [
        jnp.dot(row_block, weight, preferred_element_type=jnp.float32)
        for weight in (w_query, w_key, w_value, w_out_gate, beta_cols, decay_cols)
    ]
    summand = jnp.concatenate(results, axis=1)
    projected = lax.psum_scatter(
        summand.astype(jnp.bfloat16), "kv", scatter_dimension=0, tiled=True
    ).astype(jnp.float32)
    projected = projected * lax.dynamic_slice_in_dim(row_scale, own_first, own_rows, 0)[:, None]
    mixed, next_state = mixer_core(
        projected[:, :width_dev],
        projected[:, width_dev : 2 * width_dev],
        projected[:, 2 * width_dev : 3 * width_dev],
        projected[:, 3 * width_dev : 4 * width_dev],
        projected[:, 4 * width_dev : 4 * width_dev + head_count],
        projected[:, 4 * width_dev + head_count :],
        delta_state,
        decay_rate,
        head_gain,
    )
    attn_part = jnp.dot(
        lax.all_gather(mixed, "kv", axis=0, tiled=True), w_mix, preferred_element_type=jnp.float32
    )
    attn = lax.psum_scatter(
        attn_part.astype(jnp.bfloat16), "tp", scatter_dimension=1, tiled=True
    ).astype(jnp.float32)
    middle_own = (token_float + attn).astype(jnp.bfloat16)
    middle_float = middle_own.astype(jnp.float32)
    mid_squares = jnp.sum(middle_float * middle_float, axis=1, keepdims=True)
    gain_own = lax.dynamic_slice_in_dim(gain_mid, core_pos * feature_count, feature_count, 0)
    normed_own = (middle_float * gain_own.astype(jnp.float32)).astype(jnp.bfloat16)
    normed_half, square_parts = (
        lax.all_gather(normed_own, "kv", axis=1, tiled=True),
        lax.all_gather(mid_squares.astype(jnp.bfloat16), "kv", axis=1, tiled=True).astype(
            mid_squares.dtype
        ),
    )
    mid_total = lax.psum(jnp.sum(square_parts, axis=1), "tp")
    mid_scale = lax.rsqrt(mid_total / D + norm_epsilon)
    hidden_dev = w_gate.shape[1]
    row_block = normed_half
    summand = jnp.concatenate(
        [
            jnp.dot(row_block, w_gate, preferred_element_type=jnp.float32),
            jnp.dot(row_block, w_up, preferred_element_type=jnp.float32),
        ],
        axis=1,
    )
    gate_up = lax.psum(summand.astype(jnp.bfloat16), "tp").astype(jnp.float32)
    gate_up = gate_up * mid_scale[:, None]
    activated = (jax.nn.silu(gate_up[:, :hidden_dev]) * gate_up[:, hidden_dev:]).astype(
        jnp.bfloat16
    )
    down_local = jnp.dot(activated, w_down, preferred_element_type=jnp.float32)
    down_part = lax.psum_scatter(
        down_local.astype(jnp.bfloat16), "kv", scatter_dimension=1, tiled=True
    ).astype(jnp.float32)
    layer_out = (middle_float + down_part).astype(jnp.bfloat16)
    return (layer_out, next_state)


F32 = jnp.float32
BF16 = jnp.bfloat16
MESH = pl.DeviceIdType.MESH


def by_column(left, right):
    return lax.dot_general(
        left, right, (((1,), (1,)), ((), ())), preferred_element_type=jnp.float32
    )


def as_row(matrix):
    matrix = matrix.astype(jnp.float32)
    return jnp.concatenate([matrix[i : i + 1] for i in range(matrix.shape[0])], axis=1)


def layer_kernel(
    G,
    decay_hbm,
    head_hbm,
    gain_in_hbm,
    gain_mid_hbm,
    tokens,
    delta_state,
    w_query,
    w_key,
    w_value,
    w_out_gate,
    w_beta,
    w_decay,
    w_mix,
    w_gate,
    w_up,
    w_down,
    layer_out,
    next_state,
    tok,
    state,
    wq,
    wk,
    wv,
    wg,
    wb,
    wd,
    wm,
    wgate,
    wup,
    wdown,
    part,
    proj_out,
    proj_in,
    extra_out,
    extra_in,
    gain_out,
    gain_all,
    col_k,
    col_q,
    vec,
    mixed_all,
    wm_two,
    mid_all,
    middle,
    acc,
    gu_out,
    gu_in,
    sq_out,
    sq_in,
    down_out,
    down_in,
    gain_row_in,
    gain_row_mid,
    decay_rate,
    head_gain,
    gain_in,
    gain_mid,
    load_sem,
    tok_sem,
    gain_sem,
    proj_sem,
    extra_sem,
    mixed_sem,
    attn_sem,
    mid_sem,
    gu_sem,
    sq_sem,
    down_sem,
):
    k = lax.axis_index("kv")
    t = lax.axis_index("tp")
    other = 1 - t
    R, F = tokens.shape
    own = R // G
    C = w_query.shape[1]
    H = C // HEAD_DIM
    HEADS = w_beta.shape[0]
    HID = w_gate.shape[1]
    partner = {"tp": other}
    upper = lax.div(k, G // 2)

    def above(a, b):
        return lax.div(a - b + G - 1, G)

    def far(j):
        down = G - 1 - j
        return (1 - upper) * (down - 1 + above(down, k)) + upper * (j + 1 - above(k, j))

    others = [far(j) for j in range(G - 1)]
    nearest = others[::-1]

    loads = []

    def load(src, dst):
        copy = pltpu.make_async_copy(src, dst, load_sem.at[len(loads)])
        copy.start()
        loads.append(copy)
        return copy

    def remote(src, dst, sems, slot_send, slot_recv, device):
        return pltpu.make_async_remote_copy(
            src_ref=src,
            dst_ref=dst,
            send_sem=sems.at[0, slot_send],
            recv_sem=sems.at[1, slot_recv],
            device_id=device,
            device_id_type=MESH,
        )

    load_tok = load(tokens, tok.at[t])
    load_small = [
        load(a, b)
        for a, b in (
            (gain_in_hbm, gain_in),
            (gain_mid_hbm, gain_mid),
            (head_hbm, head_gain),
            (decay_hbm, decay_rate),
        )
    ]
    barrier = pltpu.get_barrier_semaphore()
    pl.semaphore_signal(barrier, inc=1, device_id=partner, device_id_type=MESH)
    for dst in others:
        for core in (t, other):
            pl.semaphore_signal(
                barrier, inc=1, device_id={"kv": dst, "tp": core}, device_id_type=MESH
            )
    load_proj = [
        load(a, b)
        for a, b in (
            (w_query, wq),
            (w_key, wk),
            (w_value, wv),
            (w_out_gate, wg),
            (w_beta, wb),
            (w_decay, wd),
        )
    ]

    for copy in load_small:
        copy.wait()
    gain_row_in[...] = as_row(gain_in[...])
    gain_row_mid[...] = as_row(gain_mid[...])
    gain_mid_own = gain_row_mid[:, pl.ds(pl.multiple_of(t * F, F), F)]
    gain_out[...] = jnp.broadcast_to(gain_mid_own, gain_out.shape)
    gain_all[k] = jnp.broadcast_to(gain_mid_own, gain_out.shape)
    load_tok.wait()
    pl.semaphore_wait(barrier, 2 * G - 1)

    send_tok = remote(tok.at[t], tok.at[t], tok_sem, 0, 0, partner)
    send_tok.start()
    gain_copies = []
    for j, dst in enumerate(others):
        copy = remote(gain_out, gain_all.at[k], gain_sem, j, k, {"kv": dst})
        copy.start()
        gain_copies.append(copy)

    weights = (wq, wk, wv, wg)

    def rows_of(half):
        return pl.ds(pl.multiple_of(half * F, F), F)

    def scaled(half):
        x = tok[half].astype(F32)
        gain = gain_row_in[:, rows_of(half)]
        return (x * gain).astype(BF16), jnp.sum(x * x, axis=1, keepdims=True)

    x_own, sq_own = scaled(t)
    for copy, i in zip(load_proj, range(6)):
        copy.wait()
        if i < 4:
            part[:, i * C : (i + 1) * C] = jnp.dot(
                x_own, weights[i][rows_of(t), :], preferred_element_type=F32
            )
    load_mix = load(w_mix, wm)
    load_state = load(delta_state, state)
    load_gate = load(w_gate, wgate)
    load_up = load(w_up, wup)
    load_down = load(w_down, wdown)
    beta_own = by_column(x_own, wb[:, rows_of(t)])
    decay_own = by_column(x_own, wd[:, rows_of(t)])

    remote(tok.at[t], tok.at[other], tok_sem, 0, 0, partner).wait_recv()
    x_two, sq_two = scaled(other)
    extra = jnp.zeros((R, 128), F32)
    extra_out[...] = extra.reshape(G, own, 128)
    beta = beta_own + by_column(x_two, wb[:, rows_of(other)])
    decay = decay_own + by_column(x_two, wd[:, rows_of(other)])
    extra_out[:, :, 0:HEADS] = beta.reshape(G, own, HEADS)
    extra_out[:, :, HEADS : 2 * HEADS] = decay.reshape(G, own, HEADS)
    extra_out[:, :, 2 * HEADS : 2 * HEADS + 1] = (sq_own + sq_two).reshape(G, own, 1)
    proj_copies = []
    for chunk in range(2):
        for j in range(2):
            i = 2 * chunk + j
            cols = slice(i * C, (i + 1) * C)
            value = part[:, cols] + jnp.dot(
                x_two, weights[i][rows_of(other), :], preferred_element_type=F32
            )
            part[:, cols] = value
            proj_out[chunk, :, :, j * C : (j + 1) * C] = value.astype(BF16).reshape(G, own, C)
        for j, dst in enumerate(others):
            copy = remote(
                proj_out.at[chunk, dst],
                proj_in.at[chunk, k],
                proj_sem,
                chunk * G + j,
                chunk * G + k,
                {"kv": dst},
            )
            copy.start()
            proj_copies.append(copy)
            if chunk == 0:
                copy = remote(extra_out.at[dst], extra_in.at[k], extra_sem, j, k, {"kv": dst})
                copy.start()
                proj_copies.append(copy)
    load_mix.wait()
    send_mix = remote(
        wm.at[:, pl.ds(pl.multiple_of(other * F, F), F)], wm_two, attn_sem, 0, 0, partner
    )
    send_mix.start()
    own_rows = pl.ds(pl.multiple_of(k * own, own), own)
    sum_extra = extra_out[k]
    for src in nearest:
        remote(extra_out.at[0], extra_in.at[src], extra_sem, 0, src, partner).wait_recv()
        sum_extra = sum_extra + extra_in[src]
    lane = lax.broadcasted_iota(jnp.int32, (own, 128), 1)

    def lane_of(column):
        return jnp.sum(jnp.where(lane == column, sum_extra, 0.0), axis=1, keepdims=True)

    row_scale = lax.rsqrt(lane_of(2 * HEADS) / D + norm_epsilon)

    def chunk_sum(chunk):
        total = part[own_rows, 2 * chunk * C : 2 * (chunk + 1) * C]
        for src in nearest:
            remote(
                proj_out.at[chunk, 0],
                proj_in.at[chunk, src],
                proj_sem,
                chunk * G,
                chunk * G + src,
                partner,
            ).wait_recv()
            total = total + proj_in[chunk, src].astype(F32)
        return total * row_scale

    query_key = chunk_sum(0)
    for h in range(H):
        cols = slice(h * HEAD_DIM, (h + 1) * HEAD_DIM)
        query = unit_rows(jax.nn.silu(query_key[:, cols])) * HEAD_DIM ** (-0.5)
        key_vec = unit_rows(jax.nn.silu(query_key[:, C + h * HEAD_DIM : C + (h + 1) * HEAD_DIM]))
        col_q[h] = query.T
        col_k[h] = key_vec.T
        vec[0, h] = jnp.broadcast_to(
            jnp.sum(query * key_vec, axis=1, keepdims=True), (own, HEAD_DIM)
        )
        vec[1, h] = jnp.broadcast_to(jax.nn.sigmoid(lane_of(t * H + h) * row_scale), (own, HEAD_DIM))
        pre = lane_of(HEADS + t * H + h) * row_scale
        softplus = jnp.maximum(pre, 0.0) + jnp.log1p(jnp.exp(-jnp.abs(pre)))
        vec[2, h] = jnp.broadcast_to(jnp.exp(-decay_rate[h] * softplus), (own, HEAD_DIM))
    load_state.wait()

    def recall(h, carry):
        kc, qc = col_k[h], col_q[h]
        recalled, asked = [], []
        for s in range(own):
            block = state[s, h]
            recalled.append(jnp.sum(block * kc[:, s : s + 1], axis=0, keepdims=True))
            asked.append(jnp.sum(block * qc[:, s : s + 1], axis=0, keepdims=True))
        vec[3, h] = jnp.concatenate(recalled, axis=0)
        vec[4, h] = jnp.concatenate(asked, axis=0)
        return carry

    lax.fori_loop(0, H, recall, 0, unroll=True)
    value_gate = chunk_sum(1)
    gain_row = head_gain[...]
    for h in range(H):
        cols = slice(h * HEAD_DIM, (h + 1) * HEAD_DIM)
        value_vec = jax.nn.silu(value_gate[:, cols])
        gate = jax.nn.silu(value_gate[:, C + h * HEAD_DIM : C + (h + 1) * HEAD_DIM])
        keep = vec[2, h]
        correction = vec[1, h] * (value_vec - keep * vec[3, h])
        readout = keep * vec[4, h] + vec[0, h] * correction
        vec[3, h] = correction
        readout = readout * lax.rsqrt(
            jnp.mean(readout * readout, axis=-1, keepdims=True) + norm_epsilon
        )
        mixed_all[t, k, :, cols] = (readout * gain_row * gate).astype(BF16)
    mixed_copies = []
    for j, dst in enumerate(others):
        for c, core in enumerate((t, other)):
            copy = remote(
                mixed_all.at[t, k],
                mixed_all.at[t, k],
                mixed_sem,
                2 * j + c,
                t * G + k,
                {"kv": dst, "tp": core},
            )
            copy.start()
            mixed_copies.append(copy)
    copy = remote(
        mixed_all.at[t, k], mixed_all.at[t, k], mixed_sem, 2 * G - 2, t * G + k, partner
    )
    copy.start()
    mixed_copies.append(copy)

    def update(h, carry):
        kc = col_k[h]
        keep, correction = vec[2, h], vec[3, h]
        for s in range(own):
            next_state[s, h] = (
                keep[s : s + 1] * state[s, h] + kc[:, s : s + 1] * correction[s : s + 1]
            )
        return carry

    lax.fori_loop(0, H, update, 0, unroll=True)
    send_mix.wait_recv()

    def half_product(core, sources, weight):
        for src in sources:
            remote(
                mixed_all.at[t, k], mixed_all.at[core, src], mixed_sem, 0, core * G + src, partner
            ).wait_recv()
        mixed = jnp.concatenate([mixed_all[core, j].astype(F32) for j in range(G)], axis=0)
        product = jnp.dot(mixed.astype(BF16), weight, preferred_element_type=F32)
        return product.astype(BF16).astype(F32)

    attn = half_product(t, nearest, wm[:, pl.ds(pl.multiple_of(t * F, F), F)])
    attn = attn + half_product(other, [k] + nearest, wm_two[...])
    mid = (tok[t].astype(F32) + attn).astype(BF16)
    middle[...] = mid
    mid_all[k] = mid
    mid_copies = []
    for j, dst in enumerate(others):
        copy = remote(middle, mid_all.at[k], mid_sem, j, k, {"kv": dst})
        copy.start()
        mid_copies.append(copy)

    cut = (HID // 128 + 1) // 2 * 128
    spans = (slice(0, cut), slice(cut, HID))
    squares = jnp.zeros((R, 1), F32)
    load_gate.wait()
    load_up.wait()
    for src in nearest:
        remote(gain_out, gain_all.at[src], gain_sem, 0, src, partner).wait_recv()
    gu_copies = []
    for position, src in enumerate([k] + nearest):
        if position:
            remote(middle, mid_all.at[src], mid_sem, 0, src, partner).wait_recv()
        x = mid_all[src].astype(F32)
        squares = squares + jnp.sum(x * x, axis=1, keepdims=True)
        x = (x * gain_all[src][0:1]).astype(BF16)
        rows = pl.ds(pl.multiple_of(src * F, F), F)
        last = position == G - 1
        if last:
            sq_out[...] = jnp.broadcast_to(squares, sq_out.shape)
            send_sq = remote(sq_out, sq_in, sq_sem, 0, 0, partner)
            send_sq.start()
        for c, span in enumerate(spans):
            for j, w in enumerate((wgate, wup)):
                value = jnp.dot(x, w[rows, span], preferred_element_type=F32)
                if position:
                    value = acc[j, :, span] + value
                acc[j, :, span] = value
                if last:
                    gu_out[j, :, span] = value.astype(BF16)
            if last:
                copy = remote(
                    gu_out.at[:, :, span], gu_in.at[:, :, span], gu_sem, c, c, partner
                )
                copy.start()
                gu_copies.append(copy)
    send_sq.wait_recv()
    mid_scale = lax.rsqrt((squares + sq_in[:, 0:1]) / D + norm_epsilon)
    pieces = []
    for c, span in enumerate(spans):
        gu_copies[c].wait_recv()
        gate = (acc[0, :, span] + gu_in[0, :, span].astype(F32)) * mid_scale
        up = (acc[1, :, span] + gu_in[1, :, span].astype(F32)) * mid_scale
        pieces.append((jax.nn.silu(gate) * up).astype(BF16))
    load_down.wait()
    down_copies = []
    for j, dst in enumerate(others + [k]):
        cols = pl.ds(pl.multiple_of(dst * F, F), F)
        value = sum(
            jnp.dot(piece, wdown[span, cols], preferred_element_type=F32)
            for piece, span in zip(pieces, spans)
        )
        if j < G - 1:
            down_out[j] = value.astype(BF16)
            copy = remote(down_out.at[j], down_in.at[k], down_sem, j, k, {"kv": dst})
            copy.start()
            down_copies.append(copy)
    total = value
    for src in nearest:
        remote(down_out.at[0], down_in.at[src], down_sem, 0, src, partner).wait_recv()
        total = total + down_in[src].astype(F32)
    layer_out[...] = (middle[...].astype(F32) + total).astype(BF16)
    send_tok.wait_send()
    for copy in gain_copies + proj_copies + mixed_copies + mid_copies + gu_copies + down_copies:
        copy.wait_send()
    send_mix.wait_send()
    send_sq.wait_send()


def one_kernel(
    tokens,
    delta_state,
    gain_in,
    w_query,
    w_key,
    w_value,
    w_out_gate,
    w_beta,
    w_decay,
    decay_rate,
    head_gain,
    w_mix,
    gain_mid,
    w_gate,
    w_up,
    w_down,
):
    G = lax.axis_size("kv")
    R, F = tokens.shape
    own = R // G
    C = w_query.shape[1]
    H = C // HEAD_DIM
    HID = w_gate.shape[1]
    vmem = lambda like: pltpu.VMEM(like.shape, like.dtype)
    dma = pltpu.SemaphoreType.DMA
    anywhere = pl.BlockSpec(memory_space=pl.ANY)
    inside = pl.BlockSpec(memory_space=pltpu.VMEM)
    return pl.pallas_call(
        functools.partial(layer_kernel, G),
        out_shape=(
            pltpu.VMEM(tokens.shape, BF16),
            pltpu.VMEM(delta_state.shape, F32),
        ),
        in_specs=[anywhere] * 16,
        out_specs=(inside, inside),
        scratch_shapes=[
            pltpu.VMEM((2, R, F), BF16),
            vmem(delta_state),
            vmem(w_query),
            vmem(w_key),
            vmem(w_value),
            vmem(w_out_gate),
            pltpu.VMEM(w_beta.shape[::-1], BF16),
            pltpu.VMEM(w_decay.shape[::-1], BF16),
            vmem(w_mix),
            vmem(w_gate),
            vmem(w_up),
            vmem(w_down),
            pltpu.VMEM((R, 4 * C), F32),
            pltpu.VMEM((2, G, own, 2 * C), BF16),
            pltpu.VMEM((2, G, own, 2 * C), BF16),
            pltpu.VMEM((G, own, 128), F32),
            pltpu.VMEM((G, own, 128), F32),
            pltpu.VMEM((8, F), F32),
            pltpu.VMEM((G, 8, F), F32),
            pltpu.VMEM((H, HEAD_DIM, own), F32),
            pltpu.VMEM((H, HEAD_DIM, own), F32),
            pltpu.VMEM((5, H, own, HEAD_DIM), F32),
            pltpu.VMEM((2, G, own, C), BF16),
            pltpu.VMEM((C, F), BF16),
            pltpu.VMEM((G, R, F), BF16),
            pltpu.VMEM((R, F), BF16),
            pltpu.VMEM((2, R, HID), F32),
            pltpu.VMEM((2, R, HID), BF16),
            pltpu.VMEM((2, R, HID), BF16),
            pltpu.VMEM((R, 128), F32),
            pltpu.VMEM((R, 128), F32),
            pltpu.VMEM((G - 1, R, F), BF16),
            pltpu.VMEM((G, R, F), BF16),
            pltpu.VMEM((1, 2 * F), F32),
            pltpu.VMEM((1, 2 * F), F32),
            pltpu.SMEM((H,), F32),
            pltpu.VMEM((1, HEAD_DIM), F32),
            pltpu.VMEM((2 * F // 128, 128), BF16),
            pltpu.VMEM((2 * F // 128, 128), BF16),
            dma((16,)),
            dma((2, 1)),
            dma((2, G)),
            dma((2, 2 * G)),
            dma((2, G)),
            dma((2, 2 * G)),
            dma((2, 1)),
            dma((2, G)),
            dma((2, 2)),
            dma((2, 1)),
            dma((2, G)),
        ],
        compiler_params=pltpu.CompilerParams(
            collective_id=0, has_side_effects=True, vmem_limit_bytes=60 * 2**20
        ),
    )(
        decay_rate,
        head_gain.reshape(1, -1),
        gain_in.reshape(-1, 128),
        gain_mid.reshape(-1, 128),
        tokens,
        delta_state,
        w_query,
        w_key,
        w_value,
        w_out_gate,
        w_beta.T,
        w_decay.T,
        w_mix,
        w_gate,
        w_up,
        w_down,
    )


def step(*args):
    tokens, w_query, w_gate = args[0], args[3], args[13]
    rows, features = tokens.shape
    aligned = features % 128 == 0 and w_gate.shape[1] % 128 == 0
    aligned = aligned and w_query.shape[1] % HEAD_DIM == 0 and w_query.shape[0] == 2 * features
    aligned = aligned and rows % (8 * lax.axis_size("kv")) == 0 and lax.axis_size("tp") == 2
    return one_kernel(*args) if aligned else local(*args)


def solution(mesh):
    in_specs = (
        P("dp", ("kv", "tp")),
        P(("dp", "kv"), "tp", None, None),
        P("kv"),
        P("kv", "tp"),
        P("kv", "tp"),
        P("kv", "tp"),
        P("kv", "tp"),
        P("kv", None),
        P("kv", None),
        P("tp"),
        P(),
        P("tp", "kv"),
        P("kv"),
        P("tp", "kv"),
        P("tp", "kv"),
        P("kv", "tp"),
    )
    out_specs = (P("dp", ("kv", "tp")), P(("dp", "kv"), "tp", None, None))
    return jax.shard_map(step, mesh=mesh, in_specs=in_specs, out_specs=out_specs, check_vma=False)
```
